512 devices in a mesh: fs: 64 (over z, y), tp: 8 (over x, core).
Axes of the slice: x: 4, y: 4, z: 16, core: 2. Of those that a mesh axis runs over, the one named last changes fastest.
Arguments:
- normed_input: bfloat16 [32768, 4096], P('fs', 'tp'), may hold values from -16 to 16
- value_cotangent: bfloat16 [32768, 2048], P('fs', 'tp'), may hold values from -0.005859375 to 0.005859375
- mixer_output: bfloat16 [32768, 2048], P('fs', 'tp'), may hold values from -6 to 6
- output_cotangent: bfloat16 [32768, 4096], P('fs', 'tp'), may hold values from -0.0078125 to 0.0078125
- value_factor: bfloat16 [4096, 128], replicated, may hold values from -0.5 to 0.5
- output_factor: bfloat16 [2048, 128], replicated, may hold values from -0.5 to 0.5
- value_master: float32 [4096, 2048], P('fs', 'tp'), may hold values from -0.09375 to 0.09375
- value_moment: float32 [128, 2048], P(None, 'tp'), may hold values from -6 to 6
- value_second: float32 [128, 2048], P(None, 'tp'), may hold values from 0.0625 to 16, as said below
- output_master: float32 [2048, 4096], P('fs', 'tp'), may hold values from -0.125 to 0.125
- output_moment: float32 [128, 4096], P(None, 'tp'), may hold values from -6 to 6
- output_second: float32 [128, 4096], P(None, 'tp'), may hold values from 0.0625 to 16, as said below
Outputs:
- value_step: float32 [4096, 2048], P('fs', 'tp')
- value_new: float32 [4096, 2048], P('fs', 'tp')
- value_copy: bfloat16 [4096, 2048], P(None, 'tp')
- value_moment_new: float32 [128, 2048], P(None, 'tp')
- value_second_new: float32 [128, 2048], P(None, 'tp')
- output_step: float32 [2048, 4096], P('fs', 'tp')
- output_new: float32 [2048, 4096], P('fs', 'tp')
- output_copy: bfloat16 [2048, 4096], P(None, 'tp')
- output_moment_new: float32 [128, 4096], P(None, 'tp')
- output_second_new: float32 [128, 4096], P(None, 'tp')
The draws below stay inside these ranges and needn't reach their ends.
Inputs may be any that keep to these rules, and one draw needn't show every extreme that they name: `value_second`: positive, with a scale that differs between groups of columns. `output_second`: positive, with a scale that differs between groups of columns.
All inputs are finite; a program needn't handle non-finite values.
Results may differ from the reference program's by a relative error of at most 0.004.
Values may be sent and summed in bfloat16 or wider, within the bound.
No kernel may reach another device: no remote copies, remote signals or barrier semaphores. Data moves between devices by JAX's collectives and lax.ppermute only.
A program may use at most 64 MiB of HBM per device.

```python
import math
import jax
import jax.numpy as jnp
from jax import lax

D = 4096
WIDTH = 2048
R = 128
TOK_DEV = 512
TOKENS = 32768
N_FS = 64
N_TP = 8


def second_draw(key, rows, columns):
    levels = jnp.exp(jax.random.uniform(jax.random.fold_in(key, 11), (rows, columns), jnp.float32, math.log(0.25), math.log(4.0)))
    groups = jnp.exp(jax.random.uniform(jax.random.fold_in(key, 12), (16,), jnp.float32, math.log(0.25), math.log(4.0)))
    return levels * jnp.repeat(groups, columns // 16)[None, :]


def draw_value_second(key, part):
    return second_draw(jax.random.fold_in(key, 1), R, WIDTH)


def draw_output_second(key, part):
    return second_draw(jax.random.fold_in(key, 2), R, D)


def strengthened(array, rng, source, target, parts, factor):
    def block_of(axis_at):
        return (jnp.arange(array.shape[axis_at]) // (array.shape[axis_at] // parts)).reshape((-1,) + (1,) * (array.ndim - 1 - axis_at))

    near = jax.random.permutation(rng, parts)[block_of(target)]
    other_side = (block_of(target) + parts // 2) % parts
    return jnp.where((block_of(source) == near) | (block_of(source) == other_side), factor * array, array)


def block_levels(own_key, extent, split, least, top_value):
    def one(axis_at, parts):
        draws = jax.random.uniform(jax.random.fold_in(jax.random.fold_in(own_key, 6), axis_at), (parts,), jnp.float32, least / len(split), top_value / len(split))
        return jnp.repeat(jnp.exp(draws), extent[axis_at] // parts).reshape((-1,) + (1,) * (len(extent) - axis_at - 1))

    factor_of = one(*split[0])
    for cut in split[1:]:
        factor_of = factor_of * one(*cut)
    return factor_of


def noise(key, extent, width, reach, pieces=(), dtype=jnp.bfloat16):
    result = width * jax.random.normal(key, extent, jnp.float32)
    if pieces:
        result = result * block_levels(key, extent, pieces, -0.22, 0.18)
    return jnp.clip(result, -reach, reach).astype(dtype)


def gaussian_with(key, dims, scale, bound, shards, heavy, held_as=jnp.bfloat16):
    array = scale * jax.random.normal(key, dims, jnp.float32)
    if shards:
        array = array * block_levels(key, dims, shards, -0.22, 0.18)
    return jnp.clip(strengthened(array, jax.random.fold_in(key, 3), *heavy), -bound, bound).astype(held_as)


def setup_inputs(seed: int = 0) -> dict:
    streams_of = jax.random.split(jax.random.key(seed), 13)
    return {
        "normed_input": gaussian_with(streams_of[0], (TOKENS, D), 1.0, 16.0, ((0, 64), (1, 8)), (0, 1, 64, 4.0)),
        "value_cotangent": noise(streams_of[1], (TOKENS, WIDTH), ((R / (D * TOK_DEV * N_FS)) ** 0.5), 0.005859375, ((0, 64), (1, 8))),
        "mixer_output": noise(streams_of[2], (TOKENS, WIDTH), 1.0, 6.0, ((0, 64), (1, 8))),
        "output_cotangent": noise(streams_of[3], (TOKENS, D), ((R / (WIDTH * TOK_DEV * N_FS)) ** 0.5), 0.0078125, ((0, 64), (1, 8))),
        "value_factor": noise(streams_of[4], (D, R), R ** -0.5, 0.5),
        "output_factor": noise(streams_of[5], (WIDTH, R), R ** -0.5, 0.5),
        "value_master": noise(streams_of[6], (D, WIDTH), D ** -0.5, 0.09375, ((0, 64), (1, 8)), jnp.float32),
        "value_moment": noise(streams_of[7], (R, WIDTH), 1.0, 6.0, ((1, 8),), jnp.float32),
        "value_second": draw_value_second(jax.random.fold_in(streams_of[12], 71), 0),
        "output_master": noise(streams_of[9], (WIDTH, D), WIDTH ** -0.5, 0.125, ((0, 64), (1, 8)), jnp.float32),
        "output_moment": noise(streams_of[10], (R, D), 1.0, 6.0, ((1, 8),), jnp.float32),
        "output_second": draw_output_second(jax.random.fold_in(streams_of[12], 71), 0),
    }


BETA_ONE = 0.8
BETA_TWO = 0.9
EPSILON = 1e-08
STEP_RATE = 0.005
FLOOR = 0.25

def moments(first, second, projected):
    first_new = BETA_ONE * first + (1.0 - BETA_ONE) * projected
    second_new = BETA_TWO * second + (1.0 - BETA_TWO) * projected * projected
    normalized = first_new / (jnp.sqrt(second_new) + EPSILON)
    return (first_new, second_new, normalized)

def reference(normed_input, value_cotangent, mixer_output, output_cotangent, value_factor, output_factor, value_master, value_moment, value_second, output_master, output_moment, output_second):
    highest = lax.Precision.HIGHEST
    input_reduced = jnp.dot(normed_input.astype(jnp.float32), value_factor.astype(jnp.float32), precision=highest)
    value_projected = jnp.dot(input_reduced.T, value_cotangent.astype(jnp.float32), precision=highest)
    split_cols = WIDTH // N_TP
    mixer_blocks = mixer_output.astype(jnp.float32).reshape(TOKENS, N_TP, split_cols)
    factor_blocks = output_factor.astype(jnp.float32).reshape(N_TP, split_cols, R)
    partials = jnp.einsum('tnc,ncr->ntr', mixer_blocks, factor_blocks, precision=highest).astype(jnp.bfloat16)
    partials = lax.optimization_barrier(partials)
    mixer_reduced = lax.optimization_barrier(jnp.sum(partials.astype(jnp.float32), axis=0)).astype(jnp.bfloat16)
    output_projected = jnp.dot(mixer_reduced.astype(jnp.float32).T, output_cotangent.astype(jnp.float32), precision=highest)
    value_moment_new, value_second_new, value_norm = moments(value_moment, value_second, value_projected)
    output_moment_new, output_second_new, output_norm = moments(output_moment, output_second, output_projected)
    value_scale = lax.rsqrt(jnp.mean(value_norm * value_norm) + FLOOR)
    output_scale = lax.rsqrt(jnp.mean(output_norm * output_norm) + FLOOR)
    value_step = value_scale * jnp.dot(value_factor.astype(jnp.float32), value_norm, precision=highest)
    output_step = output_scale * jnp.dot(output_factor.astype(jnp.float32), output_norm, precision=highest)
    value_new = value_master - STEP_RATE * value_step
    output_new = output_master - STEP_RATE * output_step
    return (value_step, value_new, value_new.astype(jnp.bfloat16), value_moment_new, value_second_new, output_step, output_new, output_new.astype(jnp.bfloat16), output_moment_new, output_second_new)
```

```python
import jax
import jax.numpy as jnp
from jax import lax
from jax.experimental import pallas as pl
from jax.experimental.pallas import tpu as pltpu
from jax.sharding import Mesh
from jax.sharding import PartitionSpec as P

D = 4096
WIDTH = 2048
R = 128
FS = ("zh", "zl", "y")
Z = ("zh", "zl")
NEAR = ("zl", "y")
FAR = "zh"

BETA_ONE = 0.8
BETA_TWO = 0.9
EPSILON = 1e-08
STEP_RATE = 0.005
FLOOR = 0.25


def sent_to_all(shard, axis):
    copies = jnp.broadcast_to(shard, (lax.axis_size(axis), *shard.shape))
    return lax.all_to_all(copies, axis, split_axis=0, concat_axis=0, tiled=True)


def contract_rows(left, right):
    return lax.dot_general(
        left, right, (((0,), (0,)), ((), ())), preferred_element_type=jnp.float32
    )


def moments(first, second, projected):
    first_new = BETA_ONE * first + (1.0 - BETA_ONE) * projected
    second_new = BETA_TWO * second + (1.0 - BETA_TWO) * projected * projected
    normalized = first_new / (jnp.sqrt(second_new) + EPSILON)
    return (first_new, second_new, normalized)


def split(scaled):
    high = scaled.astype(jnp.bfloat16)
    return high, (scaled - high.astype(jnp.float32)).astype(jnp.bfloat16)


def product(rows, high_ref, low_ref):
    return jnp.dot(rows, high_ref[...], preferred_element_type=jnp.float32) + jnp.dot(
        rows, low_ref[...], preferred_element_type=jnp.float32
    )


def update_kernel(
    scales_ref,
    masters_ref,
    value_factor_ref,
    output_factor_ref,
    value_norm_ref,
    output_norm_ref,
    value_here_ref,
    output_here_ref,
    value_master_ref,
    output_master_ref,
    value_step_ref,
    value_new_ref,
    value_copy_ref,
    output_step_ref,
    output_new_ref,
    output_copy_ref,
    value_high,
    value_low,
    output_high,
    output_low,
):
    @pl.when(pl.program_id(0) == 0)
    def _():
        value_high[...], value_low[...] = split(scales_ref[0] * value_norm_ref[...])
        output_high[...], output_low[...] = split(scales_ref[1] * output_norm_ref[...])
        step = product(value_here_ref[...], value_high, value_low)
        value_step_ref[...] = step
        value_new_ref[...] = value_master_ref[...] - STEP_RATE * step
        step = product(output_here_ref[...], output_high, output_low)
        output_step_ref[...] = step
        output_new_ref[...] = output_master_ref[...] - STEP_RATE * step

    group, packed_rows, width = masters_ref.shape
    value_rows = value_here_ref.shape[0]
    output_rows = output_here_ref.shape[0]
    step = product(value_factor_ref[...], value_high, value_low)
    old = masters_ref[:, :value_rows, :].reshape(group * value_rows, width)
    value_copy_ref[...] = (old.astype(jnp.float32) - STEP_RATE * step).astype(jnp.bfloat16)
    step = product(output_factor_ref[...], output_high, output_low)
    for side in range(2):
        first = value_rows + side * output_rows
        old = masters_ref[:, first : first + output_rows, :].reshape(group * output_rows, width)
        columns = slice(side * width, (side + 1) * width)
        output_copy_ref[:, columns] = (
            old.astype(jnp.float32) - STEP_RATE * step[:, columns]
        ).astype(jnp.bfloat16)


def updated(
    scales,
    masters,
    value_factor,
    output_factor,
    value_norm,
    output_norm,
    value_here,
    output_here,
    value_master,
    output_master,
):
    n_fs, packed_rows, width = masters.shape
    steps = 8
    group = n_fs // steps
    value_rows, value_cols = value_master.shape
    output_rows, output_cols = output_master.shape

    def whole(array):
        return pl.BlockSpec(array.shape, lambda i: (0,) * array.ndim)

    def rows(count, columns):
        return pl.BlockSpec((count, columns), lambda i: (i, 0))

    return pl.pallas_call(
        update_kernel,
        grid=(steps,),
        in_specs=[
            pl.BlockSpec(memory_space=pltpu.SMEM),
            pl.BlockSpec((group, packed_rows, width), lambda i: (i, 0, 0)),
            rows(group * value_rows, R),
            rows(group * output_rows, R),
            whole(value_norm),
            whole(output_norm),
            whole(value_here),
            whole(output_here),
            whole(value_master),
            whole(output_master),
        ],
        out_specs=[
            whole(value_master),
            whole(value_master),
            rows(group * value_rows, value_cols),
            whole(output_master),
            whole(output_master),
            rows(group * output_rows, output_cols),
        ],
        out_shape=[
            jax.ShapeDtypeStruct(value_master.shape, jnp.float32),
            jax.ShapeDtypeStruct(value_master.shape, jnp.float32),
            jax.ShapeDtypeStruct((n_fs * value_rows, value_cols), jnp.bfloat16),
            jax.ShapeDtypeStruct(output_master.shape, jnp.float32),
            jax.ShapeDtypeStruct(output_master.shape, jnp.float32),
            jax.ShapeDtypeStruct((n_fs * output_rows, output_cols), jnp.bfloat16),
        ],
        scratch_shapes=[
            pltpu.VMEM(value_norm.shape, jnp.bfloat16),
            pltpu.VMEM(value_norm.shape, jnp.bfloat16),
            pltpu.VMEM(output_norm.shape, jnp.bfloat16),
            pltpu.VMEM(output_norm.shape, jnp.bfloat16),
        ],
        cost_estimate=pl.CostEstimate(
            flops=4 * R * n_fs * (value_rows * value_cols + output_rows * output_cols),
            bytes_accessed=4 * n_fs * packed_rows * width,
            transcendentals=0,
        ),
        name="update",
    )(
        scales,
        masters,
        value_factor,
        output_factor,
        value_norm,
        output_norm,
        value_here,
        output_here,
        value_master,
        output_master,
    )


def per_device(
    normed_input,
    value_cotangent,
    mixer_output,
    output_cotangent,
    value_factor,
    output_factor,
    value_master,
    value_moment,
    value_second,
    output_master,
    output_moment,
    output_second,
):
    row_index = lax.axis_index(FS)
    column_index = lax.axis_index("tp")
    n_fs = lax.axis_size(FS)
    n_tp = lax.axis_size("tp")
    value_rows, value_cols = value_master.shape
    output_rows, output_cols = output_master.shape
    tokens, feature_cols = normed_input.shape
    head_cols = mixer_output.shape[1]
    half = output_cols // 2

    packed = jnp.concatenate(
        [value_master, output_master[:, :half], output_master[:, half:]], axis=0
    ).astype(jnp.bfloat16)
    plane = sent_to_all(packed, "y")

    factor_features = lax.dynamic_slice_in_dim(
        value_factor, column_index * feature_cols, feature_cols, 0
    )
    factor_heads = lax.dynamic_slice_in_dim(output_factor, column_index * head_cols, head_cols, 0)
    input_partial = jnp.dot(normed_input, factor_features, preferred_element_type=jnp.float32)
    mixer_partial = jnp.dot(mixer_output, factor_heads, preferred_element_type=jnp.float32)
    partial = jnp.concatenate([input_partial, mixer_partial], axis=1).astype(jnp.bfloat16)
    partial = partial.reshape(n_tp, tokens // n_tp, 2 * R)
    partial, plane = lax.optimization_barrier((partial, plane))
    masters = lax.all_gather(plane, Z).reshape(n_fs, *packed.shape)
    blocks = lax.all_to_all(partial, "tp", split_axis=0, concat_axis=0, tiled=True)
    own = jnp.sum(blocks.astype(jnp.float32), axis=0).astype(jnp.bfloat16)
    reduced = sent_to_all(own, "tp").reshape(tokens, 2 * R)

    value_partial = contract_rows(reduced[:, :R], value_cotangent)
    output_partial = contract_rows(reduced[:, R:], output_cotangent)
    n_near = lax.axis_size(NEAR)
    gradient = jnp.concatenate([value_partial, output_partial], axis=1)
    gradient = gradient.reshape(n_near, R // n_near, -1)
    gradient = lax.all_to_all(gradient, NEAR, split_axis=0, concat_axis=0, tiled=True)
    gradient = jnp.sum(gradient, axis=0)
    gradient = jnp.sum(sent_to_all(gradient, FAR), axis=0)
    gradient = sent_to_all(gradient, NEAR).reshape(R, -1)
    value_projected = gradient[:, :value_cols]
    output_projected = gradient[:, value_cols:]

    value_moment_new, value_second_new, value_norm = moments(
        value_moment, value_second, value_projected
    )
    output_moment_new, output_second_new, output_norm = moments(
        output_moment, output_second, output_projected
    )
    totals = jnp.stack([jnp.sum(value_norm * value_norm), jnp.sum(output_norm * output_norm)])
    totals = jnp.sum(sent_to_all(totals.reshape(1, 2), "tp"), axis=(0, 1))
    value_scale = lax.rsqrt(totals[0] / (R * WIDTH) + FLOOR)
    output_scale = lax.rsqrt(totals[1] / (R * D) + FLOOR)

    factor_here = lax.dynamic_slice_in_dim(value_factor, row_index * value_rows, value_rows, 0)
    output_factor_rows = lax.dynamic_slice_in_dim(
        output_factor, row_index * output_rows, output_rows, 0
    )
    scales = jnp.stack([value_scale, output_scale])
    value_step, value_new, value_copy, output_step, output_new, output_copy = updated(
        scales,
        masters,
        value_factor,
        output_factor,
        value_norm,
        output_norm,
        factor_here,
        output_factor_rows,
        value_master,
        output_master,
    )
    return (
        value_step,
        value_new,
        value_copy,
        value_moment_new,
        value_second_new,
        output_step,
        output_new,
        output_copy,
        output_moment_new,
        output_second_new,
    )


def solution(mesh):
    finer = Mesh(mesh.devices.reshape(4, 4, 4, mesh.shape["tp"]), ("zh", "zl", "y", "tp"))
    placed = (
        P(FS, "tp"),
        P(FS, "tp"),
        P(FS, "tp"),
        P(FS, "tp"),
        P(),
        P(),
        P(FS, "tp"),
        P(None, "tp"),
        P(None, "tp"),
        P(FS, "tp"),
        P(None, "tp"),
        P(None, "tp"),
    )
    return jax.shard_map(
        per_device,
        mesh=finer,
        in_specs=placed,
        out_specs=(
            P(FS, "tp"),
            P(FS, "tp"),
            P(None, "tp"),
            P(None, "tp"),
            P(None, "tp"),
            P(FS, "tp"),
            P(FS, "tp"),
            P(None, "tp"),
            P(None, "tp"),
            P(None, "tp"),
        ),
        check_vma=False,
    )
```

```python
import jax
import jax.numpy as jnp
from jax import lax
from jax.experimental import pallas as pl
from jax.experimental.pallas import tpu as pltpu
from jax.sharding import Mesh
from jax.sharding import PartitionSpec as P

D = 4096
WIDTH = 2048
R = 128
FS = ("zh", "zl", "y")
Z = ("zh", "zl")
NEAR = ("zl", "y")
FAR = "zh"

BETA_ONE = 0.8
BETA_TWO = 0.9
EPSILON = 1e-08
STEP_RATE = 0.005
FLOOR = 0.25


def sent_to_all(shard, axis):
    copies = jnp.broadcast_to(shard, (lax.axis_size(axis), *shard.shape))
    return lax.all_to_all(copies, axis, split_axis=0, concat_axis=0, tiled=True)


def summed_far(part, axis):
    size = lax.axis_size(axis)

    def shifted(by):
        return lax.ppermute(part, axis, [(i, (i + by) % size) for i in range(size)])

    opposite, before, after = shifted(2), shifted(1), shifted(3)
    return (part + opposite) + (before + after)


def contract_rows(left, right):
    return lax.dot_general(
        left, right, (((0,), (0,)), ((), ())), preferred_element_type=jnp.float32
    )


def moments(first, second, projected):
    first_new = BETA_ONE * first + (1.0 - BETA_ONE) * projected
    second_new = BETA_TWO * second + (1.0 - BETA_TWO) * projected * projected
    normalized = first_new / (jnp.sqrt(second_new) + EPSILON)
    return (first_new, second_new, normalized)


def pack_kernel(value_ref, output_ref, packed_ref):
    copies, packed_rows, width = packed_ref.shape
    value_rows = value_ref.shape[0]
    output_rows = output_ref.shape[0]
    value = value_ref[...].astype(packed_ref.dtype)
    left = output_ref[:, :width].astype(packed_ref.dtype)
    right = output_ref[:, width:].astype(packed_ref.dtype)
    for k in range(copies):
        packed_ref[k, :value_rows, :] = value
        packed_ref[k, value_rows : value_rows + output_rows, :] = left
        packed_ref[k, value_rows + output_rows :, :] = right


def packed_copies(value_master, output_master, copies):
    value_rows, width = value_master.shape
    rows = value_rows + 2 * output_master.shape[0]
    return pl.pallas_call(
        pack_kernel,
        out_shape=jax.ShapeDtypeStruct((copies, rows, width), jnp.bfloat16),
        name="pack",
    )(value_master, output_master)


def project_kernel(index_ref, input_ref, mixer_ref, features_ref, heads_ref, partial_ref):
    blocks, tokens, width = partial_ref.shape
    partial = jnp.dot(input_ref[...], features_ref[...], preferred_element_type=jnp.float32)
    partial_ref[:, :, :R] = partial.astype(jnp.bfloat16).reshape(blocks, tokens, R)
    partial = jnp.dot(mixer_ref[...], heads_ref[...], preferred_element_type=jnp.float32)
    partial_ref[:, :, R:] = partial.astype(jnp.bfloat16).reshape(blocks, tokens, R)


def projected_tokens(index, normed_input, mixer_output, value_factor, output_factor, blocks):
    tokens, features = normed_input.shape
    heads = mixer_output.shape[1]
    return pl.pallas_call(
        project_kernel,
        grid_spec=pltpu.PrefetchScalarGridSpec(
            num_scalar_prefetch=1,
            grid=(1,),
            in_specs=[
                pl.BlockSpec((tokens, features), lambda i, index: (0, 0)),
                pl.BlockSpec((tokens, heads), lambda i, index: (0, 0)),
                pl.BlockSpec((features, R), lambda i, index: (index[0], 0)),
                pl.BlockSpec((heads, R), lambda i, index: (index[0], 0)),
            ],
            out_specs=pl.BlockSpec((blocks, tokens // blocks, 2 * R), lambda i, index: (0, 0, 0)),
        ),
        out_shape=jax.ShapeDtypeStruct((blocks, tokens // blocks, 2 * R), jnp.bfloat16),
        cost_estimate=pl.CostEstimate(
            flops=2 * tokens * (features + heads) * R,
            bytes_accessed=2 * tokens * (features + heads + 2 * R),
            transcendentals=0,
        ),
        name="project",
    )(index, normed_input, mixer_output, value_factor, output_factor)


def norms_kernel(
    gradient_ref,
    value_moment_ref,
    value_second_ref,
    output_moment_ref,
    output_second_ref,
    norm_ref,
    totals_ref,
):
    value_cols = value_moment_ref.shape[1]
    gradient = gradient_ref[...].reshape(R, gradient_ref.shape[2])
    value_norm = moments(value_moment_ref[...], value_second_ref[...], gradient[:, :value_cols])[2]
    output_norm = moments(
        output_moment_ref[...], output_second_ref[...], gradient[:, value_cols:]
    )[2]
    norm_ref[:, :value_cols] = value_norm
    norm_ref[:, value_cols:] = output_norm
    copies, _, lanes = totals_ref.shape
    total = []
    for norm in (value_norm, output_norm):
        squares = jnp.sum(norm * norm, axis=0, keepdims=True)
        total.append(sum(squares[:, k : k + lanes] for k in range(0, norm.shape[1], lanes)))
    for k in range(copies):
        totals_ref[k] = jnp.zeros(totals_ref.shape[1:], jnp.float32)
        totals_ref[k, 0:1, :] = total[0]
        totals_ref[k, 1:2, :] = total[1]


def normed(gradient, value_moment, value_second, output_moment, output_second, copies):
    return pl.pallas_call(
        norms_kernel,
        out_shape=[
            jax.ShapeDtypeStruct((R, gradient.shape[2]), jnp.float32),
            jax.ShapeDtypeStruct((copies, 8, 128), jnp.float32),
        ],
        compiler_params=pltpu.CompilerParams(vmem_limit_bytes=8 << 20),
        name="norms",
    )(gradient, value_moment, value_second, output_moment, output_second)


def inverse_root(totals, row, count):
    total = jnp.sum(totals[row : row + 1, :], axis=1, keepdims=True)
    return lax.rsqrt(total / count + FLOOR)


def product(rows, pair_ref):
    return jnp.dot(
        jnp.concatenate([rows, rows], axis=1), pair_ref[...], preferred_element_type=jnp.float32
    )


def update_kernel(
    row_ref,
    totals_ref,
    norm_ref,
    value_factor_ref,
    output_factor_ref,
    value_master_ref,
    output_master_ref,
    masters_hbm,
    value_step_hbm,
    value_new_hbm,
    value_copy_hbm,
    output_step_hbm,
    output_new_hbm,
    output_copy_hbm,
    masters,
    value_copy,
    output_copy,
    value_step,
    value_new,
    output_step,
    output_new,
    value_pair,
    output_pair,
    in_sems,
    value_sems,
    output_sems,
    own_sems,
):
    chunks = in_sems.shape[0]
    n_fs, _, width = masters.shape
    group = n_fs // chunks
    value_rows, value_cols = value_master_ref.shape
    output_rows = output_master_ref.shape[0]

    def block(k):
        return pl.ds(k * group, group)

    def arriving(k):
        return pltpu.make_async_copy(
            masters_hbm.at[block(k)], masters.at[block(k)], in_sems.at[k]
        )

    def leaving_value(k):
        rows = pl.ds(k * group * value_rows, group * value_rows)
        return pltpu.make_async_copy(value_copy.at[rows], value_copy_hbm.at[rows], value_sems.at[k])

    def leaving_output(k):
        rows = pl.ds(k * group * output_rows, group * output_rows)
        return pltpu.make_async_copy(
            output_copy.at[rows], output_copy_hbm.at[rows], output_sems.at[k]
        )

    for k in range(chunks):
        arriving(k).start()

    totals = jnp.sum(totals_ref[...], axis=0)
    value_scale = inverse_root(totals, 0, R * WIDTH)
    output_scale = inverse_root(totals, 1, R * D)
    for pair, norm, scale in (
        (value_pair, norm_ref[:, :value_cols], value_scale),
        (output_pair, norm_ref[:, value_cols:], output_scale),
    ):
        scaled = (-STEP_RATE * scale) * norm
        high = scaled.astype(jnp.bfloat16)
        pair[:R, :] = high
        pair[R:, :] = (scaled - high.astype(jnp.float32)).astype(jnp.bfloat16)

    row = row_ref[0]
    value_here = value_factor_ref[pl.ds(pl.multiple_of(row * value_rows, value_rows), value_rows), :]
    change = product(value_here, value_pair)
    value_step[...] = change * (-1.0 / STEP_RATE)
    value_new[...] = value_master_ref[...] + change
    output_here = output_factor_ref[
        pl.ds(pl.multiple_of(row * output_rows, output_rows), output_rows), :
    ]
    change = product(output_here, output_pair)
    output_step[...] = change * (-1.0 / STEP_RATE)
    output_new[...] = output_master_ref[...] + change
    own = [
        pltpu.make_async_copy(value_step, value_step_hbm, own_sems.at[0]),
        pltpu.make_async_copy(value_new, value_new_hbm, own_sems.at[1]),
        pltpu.make_async_copy(output_step, output_step_hbm, own_sems.at[2]),
        pltpu.make_async_copy(output_new, output_new_hbm, own_sems.at[3]),
    ]
    for copy in own:
        copy.start()

    for k in range(chunks):
        arriving(k).wait()
        count = group * value_rows
        rows = slice(k * count, (k + 1) * count)
        mine = slice(k * group, (k + 1) * group)
        change = product(value_factor_ref[rows, :], value_pair)
        old = masters[mine, :value_rows, :].reshape(count, width)
        value_copy[rows, :] = (old.astype(jnp.float32) + change).astype(jnp.bfloat16)
        leaving_value(k).start()
        count = group * output_rows
        rows = slice(k * count, (k + 1) * count)
        change = product(output_factor_ref[rows, :], output_pair)
        for side in range(2):
            first = value_rows + side * output_rows
            old = masters[mine, first : first + output_rows, :].reshape(count, width)
            columns = slice(side * width, (side + 1) * width)
            output_copy[rows, columns] = (old.astype(jnp.float32) + change[:, columns]).astype(
                jnp.bfloat16
            )
        leaving_output(k).start()

    for copy in own:
        copy.wait()
    for k in range(chunks):
        leaving_value(k).wait()
        leaving_output(k).wait()


def updated(
    row_index, totals, masters, value_factor, output_factor, norm, value_master, output_master
):
    n_fs, packed_rows, width = masters.shape
    chunks = 4
    value_rows, value_cols = value_master.shape
    output_rows, output_cols = output_master.shape
    in_vmem = pl.BlockSpec(memory_space=pltpu.VMEM)
    anywhere = pl.BlockSpec(memory_space=pl.ANY)
    outs = [
        jax.ShapeDtypeStruct(value_master.shape, jnp.float32),
        jax.ShapeDtypeStruct(value_master.shape, jnp.float32),
        jax.ShapeDtypeStruct((n_fs * value_rows, value_cols), jnp.bfloat16),
        jax.ShapeDtypeStruct(output_master.shape, jnp.float32),
        jax.ShapeDtypeStruct(output_master.shape, jnp.float32),
        jax.ShapeDtypeStruct((n_fs * output_rows, output_cols), jnp.bfloat16),
    ]
    return pl.pallas_call(
        update_kernel,
        in_specs=[pl.BlockSpec(memory_space=pltpu.SMEM)] + [in_vmem] * 6 + [anywhere],
        out_specs=[anywhere] * 6,
        out_shape=outs,
        scratch_shapes=[
            pltpu.VMEM(masters.shape, jnp.bfloat16),
            pltpu.VMEM(outs[2].shape, jnp.bfloat16),
            pltpu.VMEM(outs[5].shape, jnp.bfloat16),
            pltpu.VMEM(value_master.shape, jnp.float32),
            pltpu.VMEM(value_master.shape, jnp.float32),
            pltpu.VMEM(output_master.shape, jnp.float32),
            pltpu.VMEM(output_master.shape, jnp.float32),
            pltpu.VMEM((2 * R, value_cols), jnp.bfloat16),
            pltpu.VMEM((2 * R, output_cols), jnp.bfloat16),
            pltpu.SemaphoreType.DMA((chunks,)),
            pltpu.SemaphoreType.DMA((chunks,)),
            pltpu.SemaphoreType.DMA((chunks,)),
            pltpu.SemaphoreType.DMA((4,)),
        ],
        cost_estimate=pl.CostEstimate(
            flops=4 * R * n_fs * (value_rows * value_cols + output_rows * output_cols),
            bytes_accessed=4 * n_fs * packed_rows * width,
            transcendentals=0,
        ),
        compiler_params=pltpu.CompilerParams(vmem_limit_bytes=57 << 20),
        name="update",
    )(
        row_index,
        totals,
        norm,
        value_factor,
        output_factor,
        value_master,
        output_master,
        masters,
    )


def per_device(
    normed_input,
    value_cotangent,
    mixer_output,
    output_cotangent,
    value_factor,
    output_factor,
    value_master,
    value_moment,
    value_second,
    output_master,
    output_moment,
    output_second,
):
    row_index = lax.axis_index(FS).reshape(1)
    column_index = lax.axis_index("tp").reshape(1)
    n_fs = lax.axis_size(FS)
    n_tp = lax.axis_size("tp")
    tokens = normed_input.shape[0]

    packed = packed_copies(value_master, output_master, lax.axis_size("y"))
    plane = lax.all_to_all(packed, "y", split_axis=0, concat_axis=0, tiled=True)

    partial = projected_tokens(
        column_index, normed_input, mixer_output, value_factor, output_factor, n_tp
    )
    partial, plane = lax.optimization_barrier((partial, plane))
    masters = lax.all_gather(plane, Z).reshape(n_fs, *packed.shape[1:])
    blocks = lax.all_to_all(partial, "tp", split_axis=0, concat_axis=0, tiled=True)
    own = jnp.sum(blocks.astype(jnp.float32), axis=0).astype(jnp.bfloat16)
    reduced = sent_to_all(own, "tp").reshape(tokens, 2 * R)

    value_partial = contract_rows(reduced[:, :R], value_cotangent)
    output_partial = contract_rows(reduced[:, R:], output_cotangent)
    n_y, n_zl = lax.axis_size("y"), lax.axis_size("zl")
    gradient = jnp.concatenate([value_partial, output_partial], axis=1)
    gradient = gradient.reshape(n_y, R // n_y, -1)
    gradient = lax.all_to_all(gradient, "y", split_axis=0, concat_axis=0, tiled=True)
    gradient = jnp.sum(gradient, axis=0).reshape(n_zl, R // n_y // n_zl, -1)
    gradient = lax.all_to_all(gradient, "zl", split_axis=0, concat_axis=0, tiled=True)
    gradient = jnp.sum(gradient, axis=0)
    gradient = summed_far(gradient, FAR)
    gradient = sent_to_all(gradient, ("y", "zl"))

    norm, totals = normed(
        gradient, value_moment, value_second, output_moment, output_second, n_tp
    )
    flat = gradient.reshape(R, -1)
    value_cols = value_master.shape[1]
    value_moment_new, value_second_new, _ = moments(
        value_moment, value_second, flat[:, :value_cols]
    )
    output_moment_new, output_second_new, _ = moments(
        output_moment, output_second, flat[:, value_cols:]
    )
    totals = lax.all_to_all(totals, "tp", split_axis=0, concat_axis=0, tiled=True)
    value_step, value_new, value_copy, output_step, output_new, output_copy = updated(
        row_index, totals, masters, value_factor, output_factor, norm, value_master, output_master
    )
    return (
        value_step,
        value_new,
        value_copy,
        value_moment_new,
        value_second_new,
        output_step,
        output_new,
        output_copy,
        output_moment_new,
        output_second_new,
    )


def solution(mesh):
    finer = Mesh(mesh.devices.reshape(4, 4, 4, mesh.shape["tp"]), ("zh", "zl", "y", "tp"))
    placed = (
        P(FS, "tp"),
        P(FS, "tp"),
        P(FS, "tp"),
        P(FS, "tp"),
        P(),
        P(),
        P(FS, "tp"),
        P(None, "tp"),
        P(None, "tp"),
        P(FS, "tp"),
        P(None, "tp"),
        P(None, "tp"),
    )
    return jax.shard_map(
        per_device,
        mesh=finer,
        in_specs=placed,
        out_specs=(
            P(FS, "tp"),
            P(FS, "tp"),
            P(None, "tp"),
            P(None, "tp"),
            P(None, "tp"),
            P(FS, "tp"),
            P(FS, "tp"),
            P(None, "tp"),
            P(None, "tp"),
            P(None, "tp"),
        ),
        check_vma=False,
    )
```

```python
import jax
import jax.numpy as jnp
from jax import lax
from jax.experimental import pallas as pl
from jax.experimental.pallas import tpu as pltpu
from jax.sharding import Mesh
from jax.sharding import PartitionSpec as P

D = 4096
WIDTH = 2048
R = 128
FS = ("zh", "zl", "y")
Z = ("zh", "zl")
NEAR = ("zl", "y")
FAR = "zh"

BETA_ONE = 0.8
BETA_TWO = 0.9
EPSILON = 1e-08
STEP_RATE = 0.005
FLOOR = 0.25


def sent_to_all(shard, axis):
    copies = jnp.broadcast_to(shard, (lax.axis_size(axis), *shard.shape))
    return lax.all_to_all(copies, axis, split_axis=0, concat_axis=0, tiled=True)


def summed_far(part, axis):
    size = lax.axis_size(axis)

    def shifted(by):
        return lax.ppermute(part, axis, [(i, (i + by) % size) for i in range(size)])

    opposite, before, after = shifted(2), shifted(1), shifted(3)
    return (part + opposite) + (before + after)


def contract_rows(left, right):
    return lax.dot_general(
        left, right, (((0,), (0,)), ((), ())), preferred_element_type=jnp.float32
    )


def moments(first, second, projected):
    first_new = BETA_ONE * first + (1.0 - BETA_ONE) * projected
    second_new = BETA_TWO * second + (1.0 - BETA_TWO) * projected * projected
    normalized = first_new / (jnp.sqrt(second_new) + EPSILON)
    return (first_new, second_new, normalized)


def pack_kernel(value_ref, output_ref, packed_ref):
    copies, packed_rows, width = packed_ref.shape
    value_rows = value_ref.shape[0]
    output_rows = output_ref.shape[0]
    value = value_ref[...].astype(packed_ref.dtype)
    left = output_ref[:, :width].astype(packed_ref.dtype)
    right = output_ref[:, width:].astype(packed_ref.dtype)
    for k in range(copies):
        packed_ref[k, :value_rows, :] = value
        packed_ref[k, value_rows : value_rows + output_rows, :] = left
        packed_ref[k, value_rows + output_rows :, :] = right


def packed_copies(value_master, output_master, copies):
    value_rows, width = value_master.shape
    rows = value_rows + 2 * output_master.shape[0]
    return pl.pallas_call(
        pack_kernel,
        out_shape=jax.ShapeDtypeStruct((copies, rows, width), jnp.bfloat16),
        name="pack",
    )(value_master, output_master)


def project_kernel(index_ref, input_ref, mixer_ref, features_ref, heads_ref, partial_ref):
    blocks, tokens, width = partial_ref.shape
    partial = jnp.dot(input_ref[...], features_ref[...], preferred_element_type=jnp.float32)
    partial_ref[:, :, :R] = partial.astype(jnp.bfloat16).reshape(blocks, tokens, R)
    partial = jnp.dot(mixer_ref[...], heads_ref[...], preferred_element_type=jnp.float32)
    partial_ref[:, :, R:] = partial.astype(jnp.bfloat16).reshape(blocks, tokens, R)


def projected_tokens(index, normed_input, mixer_output, value_factor, output_factor, blocks):
    tokens, features = normed_input.shape
    heads = mixer_output.shape[1]
    return pl.pallas_call(
        project_kernel,
        grid_spec=pltpu.PrefetchScalarGridSpec(
            num_scalar_prefetch=1,
            grid=(1,),
            in_specs=[
                pl.BlockSpec((tokens, features), lambda i, index: (0, 0)),
                pl.BlockSpec((tokens, heads), lambda i, index: (0, 0)),
                pl.BlockSpec((features, R), lambda i, index: (index[0], 0)),
                pl.BlockSpec((heads, R), lambda i, index: (index[0], 0)),
            ],
            out_specs=pl.BlockSpec((blocks, tokens // blocks, 2 * R), lambda i, index: (0, 0, 0)),
        ),
        out_shape=jax.ShapeDtypeStruct((blocks, tokens // blocks, 2 * R), jnp.bfloat16),
        cost_estimate=pl.CostEstimate(
            flops=2 * tokens * (features + heads) * R,
            bytes_accessed=2 * tokens * (features + heads + 2 * R),
            transcendentals=0,
        ),
        name="project",
    )(index, normed_input, mixer_output, value_factor, output_factor)


def norms_kernel(
    gradient_ref,
    value_moment_ref,
    value_second_ref,
    output_moment_ref,
    output_second_ref,
    norm_ref,
    totals_ref,
):
    value_cols = value_moment_ref.shape[1]
    gradient = gradient_ref[...].astype(jnp.float32).reshape(R, gradient_ref.shape[2])
    value_norm = moments(value_moment_ref[...], value_second_ref[...], gradient[:, :value_cols])[2]
    output_norm = moments(
        output_moment_ref[...], output_second_ref[...], gradient[:, value_cols:]
    )[2]
    norm_ref[:, :value_cols] = value_norm
    norm_ref[:, value_cols:] = output_norm
    copies, _, lanes = totals_ref.shape
    total = []
    for norm in (value_norm, output_norm):
        squares = jnp.sum(norm * norm, axis=0, keepdims=True)
        total.append(sum(squares[:, k : k + lanes] for k in range(0, norm.shape[1], lanes)))
    for k in range(copies):
        totals_ref[k] = jnp.zeros(totals_ref.shape[1:], jnp.float32)
        totals_ref[k, 0:1, :] = total[0]
        totals_ref[k, 1:2, :] = total[1]


def normed(gradient, value_moment, value_second, output_moment, output_second, copies):
    return pl.pallas_call(
        norms_kernel,
        out_shape=[
            jax.ShapeDtypeStruct((R, gradient.shape[2]), jnp.float32),
            jax.ShapeDtypeStruct((copies, 8, 128), jnp.float32),
        ],
        compiler_params=pltpu.CompilerParams(vmem_limit_bytes=8 << 20),
        name="norms",
    )(gradient, value_moment, value_second, output_moment, output_second)


def inverse_root(totals, row, count):
    total = jnp.sum(totals[row : row + 1, :], axis=1, keepdims=True)
    return lax.rsqrt(total / count + FLOOR)


def product(rows, pair_ref):
    return jnp.dot(
        jnp.concatenate([rows, rows], axis=1), pair_ref[...], preferred_element_type=jnp.float32
    )


def update_kernel(
    row_ref,
    totals_ref,
    norm_ref,
    value_factor_ref,
    output_factor_ref,
    value_master_ref,
    output_master_ref,
    masters_hbm,
    value_step_hbm,
    value_new_hbm,
    value_copy_hbm,
    output_step_hbm,
    output_new_hbm,
    output_copy_hbm,
    masters,
    value_copy,
    output_copy,
    value_step,
    value_new,
    output_step,
    output_new,
    value_pair,
    output_pair,
    in_sems,
    value_sems,
    output_sems,
    own_sems,
):
    chunks = in_sems.shape[0]
    n_fs, _, width = masters.shape
    group = n_fs // chunks
    value_rows, value_cols = value_master_ref.shape
    output_rows = output_master_ref.shape[0]

    def block(k):
        return pl.ds(k * group, group)

    def arriving(k):
        return pltpu.make_async_copy(
            masters_hbm.at[block(k)], masters.at[block(k)], in_sems.at[k]
        )

    def leaving_value(k):
        rows = pl.ds(k * group * value_rows, group * value_rows)
        return pltpu.make_async_copy(value_copy.at[rows], value_copy_hbm.at[rows], value_sems.at[k])

    def leaving_output(k):
        rows = pl.ds(k * group * output_rows, group * output_rows)
        return pltpu.make_async_copy(
            output_copy.at[rows], output_copy_hbm.at[rows], output_sems.at[k]
        )

    for k in range(chunks):
        arriving(k).start()

    totals = jnp.sum(totals_ref[...], axis=0)
    value_scale = inverse_root(totals, 0, R * WIDTH)
    output_scale = inverse_root(totals, 1, R * D)
    for pair, norm, scale in (
        (value_pair, norm_ref[:, :value_cols], value_scale),
        (output_pair, norm_ref[:, value_cols:], output_scale),
    ):
        scaled = (-STEP_RATE * scale) * norm
        high = scaled.astype(jnp.bfloat16)
        pair[:R, :] = high
        pair[R:, :] = (scaled - high.astype(jnp.float32)).astype(jnp.bfloat16)

    row = row_ref[0]
    value_here = value_factor_ref[pl.ds(pl.multiple_of(row * value_rows, value_rows), value_rows), :]
    change = product(value_here, value_pair)
    value_step[...] = change * (-1.0 / STEP_RATE)
    value_new[...] = value_master_ref[...] + change
    output_here = output_factor_ref[
        pl.ds(pl.multiple_of(row * output_rows, output_rows), output_rows), :
    ]
    change = product(output_here, output_pair)
    output_step[...] = change * (-1.0 / STEP_RATE)
    output_new[...] = output_master_ref[...] + change
    own = [
        pltpu.make_async_copy(value_step, value_step_hbm, own_sems.at[0]),
        pltpu.make_async_copy(value_new, value_new_hbm, own_sems.at[1]),
        pltpu.make_async_copy(output_step, output_step_hbm, own_sems.at[2]),
        pltpu.make_async_copy(output_new, output_new_hbm, own_sems.at[3]),
    ]
    for copy in own:
        copy.start()

    for k in range(chunks):
        arriving(k).wait()
        count = group * value_rows
        rows = slice(k * count, (k + 1) * count)
        mine = slice(k * group, (k + 1) * group)
        change = product(value_factor_ref[rows, :], value_pair)
        old = masters[mine, :value_rows, :].reshape(count, width)
        value_copy[rows, :] = (old.astype(jnp.float32) + change).astype(jnp.bfloat16)
        leaving_value(k).start()
        count = group * output_rows
        rows = slice(k * count, (k + 1) * count)
        change = product(output_factor_ref[rows, :], output_pair)
        for side in range(2):
            first = value_rows + side * output_rows
            old = masters[mine, first : first + output_rows, :].reshape(count, width)
            columns = slice(side * width, (side + 1) * width)
            output_copy[rows, columns] = (old.astype(jnp.float32) + change[:, columns]).astype(
                jnp.bfloat16
            )
        leaving_output(k).start()

    for copy in own:
        copy.wait()
    for k in range(chunks):
        leaving_value(k).wait()
        leaving_output(k).wait()


def updated(
    row_index, totals, masters, value_factor, output_factor, norm, value_master, output_master
):
    n_fs, packed_rows, width = masters.shape
    chunks = 4
    value_rows, value_cols = value_master.shape
    output_rows, output_cols = output_master.shape
    in_vmem = pl.BlockSpec(memory_space=pltpu.VMEM)
    anywhere = pl.BlockSpec(memory_space=pl.ANY)
    outs = [
        jax.ShapeDtypeStruct(value_master.shape, jnp.float32),
        jax.ShapeDtypeStruct(value_master.shape, jnp.float32),
        jax.ShapeDtypeStruct((n_fs * value_rows, value_cols), jnp.bfloat16),
        jax.ShapeDtypeStruct(output_master.shape, jnp.float32),
        jax.ShapeDtypeStruct(output_master.shape, jnp.float32),
        jax.ShapeDtypeStruct((n_fs * output_rows, output_cols), jnp.bfloat16),
    ]
    return pl.pallas_call(
        update_kernel,
        in_specs=[pl.BlockSpec(memory_space=pltpu.SMEM)] + [in_vmem] * 6 + [anywhere],
        out_specs=[anywhere] * 6,
        out_shape=outs,
        scratch_shapes=[
            pltpu.VMEM(masters.shape, jnp.bfloat16),
            pltpu.VMEM(outs[2].shape, jnp.bfloat16),
            pltpu.VMEM(outs[5].shape, jnp.bfloat16),
            pltpu.VMEM(value_master.shape, jnp.float32),
            pltpu.VMEM(value_master.shape, jnp.float32),
            pltpu.VMEM(output_master.shape, jnp.float32),
            pltpu.VMEM(output_master.shape, jnp.float32),
            pltpu.VMEM((2 * R, value_cols), jnp.bfloat16),
            pltpu.VMEM((2 * R, output_cols), jnp.bfloat16),
            pltpu.SemaphoreType.DMA((chunks,)),
            pltpu.SemaphoreType.DMA((chunks,)),
            pltpu.SemaphoreType.DMA((chunks,)),
            pltpu.SemaphoreType.DMA((4,)),
        ],
        cost_estimate=pl.CostEstimate(
            flops=4 * R * n_fs * (value_rows * value_cols + output_rows * output_cols),
            bytes_accessed=4 * n_fs * packed_rows * width,
            transcendentals=0,
        ),
        compiler_params=pltpu.CompilerParams(vmem_limit_bytes=52 << 20),
        name="update",
    )(
        row_index,
        totals,
        norm,
        value_factor,
        output_factor,
        value_master,
        output_master,
        masters,
    )


def per_device(
    normed_input,
    value_cotangent,
    mixer_output,
    output_cotangent,
    value_factor,
    output_factor,
    value_master,
    value_moment,
    value_second,
    output_master,
    output_moment,
    output_second,
):
    row_index = lax.axis_index(FS).reshape(1)
    column_index = lax.axis_index("tp").reshape(1)
    n_fs = lax.axis_size(FS)
    n_tp = lax.axis_size("tp")
    tokens = normed_input.shape[0]

    packed = packed_copies(value_master, output_master, lax.axis_size("y"))
    plane = lax.all_to_all(packed, "y", split_axis=0, concat_axis=0, tiled=True)

    partial = projected_tokens(
        column_index, normed_input, mixer_output, value_factor, output_factor, n_tp
    )
    partial, plane, row_index = lax.optimization_barrier((partial, plane, row_index))
    masters = lax.all_gather(plane, Z).reshape(n_fs, *packed.shape[1:])
    blocks = lax.all_to_all(partial, "tp", split_axis=0, concat_axis=0, tiled=True)
    own = jnp.sum(blocks.astype(jnp.float32), axis=0).astype(jnp.bfloat16)
    reduced = sent_to_all(own, "tp").reshape(tokens, 2 * R)

    value_partial = contract_rows(reduced[:, :R], value_cotangent)
    output_partial = contract_rows(reduced[:, R:], output_cotangent)
    n_y, n_zl = lax.axis_size("y"), lax.axis_size("zl")
    gradient = jnp.concatenate([value_partial, output_partial], axis=1)
    gradient = gradient.reshape(n_y, R // n_y, -1)
    gradient = lax.all_to_all(gradient, "y", split_axis=0, concat_axis=0, tiled=True)
    gradient = jnp.sum(gradient, axis=0).reshape(n_zl, R // n_y // n_zl, -1)
    gradient = lax.all_to_all(gradient, "zl", split_axis=0, concat_axis=0, tiled=True)
    gradient = jnp.sum(gradient, axis=0)
    gradient = summed_far(gradient, FAR)
    gradient = sent_to_all(gradient.astype(jnp.bfloat16), ("y", "zl"))

    norm, totals = normed(
        gradient, value_moment, value_second, output_moment, output_second, n_tp
    )
    flat = gradient.astype(jnp.float32).reshape(R, -1)
    value_cols = value_master.shape[1]
    value_moment_new, value_second_new, _ = moments(
        value_moment, value_second, flat[:, :value_cols]
    )
    output_moment_new, output_second_new, _ = moments(
        output_moment, output_second, flat[:, value_cols:]
    )
    totals = lax.all_to_all(totals, "tp", split_axis=0, concat_axis=0, tiled=True)
    value_step, value_new, value_copy, output_step, output_new, output_copy = updated(
        row_index, totals, masters, value_factor, output_factor, norm, value_master, output_master
    )
    return (
        value_step,
        value_new,
        value_copy,
        value_moment_new,
        value_second_new,
        output_step,
        output_new,
        output_copy,
        output_moment_new,
        output_second_new,
    )


def solution(mesh):
    finer = Mesh(mesh.devices.reshape(4, 4, 4, mesh.shape["tp"]), ("zh", "zl", "y", "tp"))
    placed = (
        P(FS, "tp"),
        P(FS, "tp"),
        P(FS, "tp"),
        P(FS, "tp"),
        P(),
        P(),
        P(FS, "tp"),
        P(None, "tp"),
        P(None, "tp"),
        P(FS, "tp"),
        P(None, "tp"),
        P(None, "tp"),
    )
    return jax.shard_map(
        per_device,
        mesh=finer,
        in_specs=placed,
        out_specs=(
            P(FS, "tp"),
            P(FS, "tp"),
            P(None, "tp"),
            P(None, "tp"),
            P(None, "tp"),
            P(FS, "tp"),
            P(FS, "tp"),
            P(None, "tp"),
            P(None, "tp"),
            P(None, "tp"),
        ),
        check_vma=False,
    )
```

```python
import jax
import jax.numpy as jnp
from jax import lax
from jax.experimental import pallas as pl
from jax.experimental.pallas import tpu as pltpu
from jax.sharding import Mesh
from jax.sharding import PartitionSpec as P

D = 4096
WIDTH = 2048
R = 128
FS = ("zh", "zl", "y")
Z = ("zh", "zl")
NEAR = ("zl", "y")
FAR = "zh"

BETA_ONE = 0.8
BETA_TWO = 0.9
EPSILON = 1e-08
STEP_RATE = 0.005
FLOOR = 0.25


def sent_to_all(shard, axis):
    copies = jnp.broadcast_to(shard, (lax.axis_size(axis), *shard.shape))
    return lax.all_to_all(copies, axis, split_axis=0, concat_axis=0, tiled=True)


def summed_far(part, axis):
    size = lax.axis_size(axis)
    for by in (size // 2, 1):
        part = part + lax.ppermute(part, axis, [(i, i ^ by) for i in range(size)])
    return part


def contract_rows(left, right):
    return lax.dot_general(
        left, right, (((0,), (0,)), ((), ())), preferred_element_type=jnp.float32
    )


def moments(first, second, projected):
    first_new = BETA_ONE * first + (1.0 - BETA_ONE) * projected
    second_new = BETA_TWO * second + (1.0 - BETA_TWO) * projected * projected
    normalized = first_new / (jnp.sqrt(second_new) + EPSILON)
    return (first_new, second_new, normalized)


def pack_kernel(value_ref, output_ref, packed_ref):
    copies, packed_rows, width = packed_ref.shape
    value_rows = value_ref.shape[0]
    output_rows = output_ref.shape[0]
    value = value_ref[...].astype(packed_ref.dtype)
    left = output_ref[:, :width].astype(packed_ref.dtype)
    right = output_ref[:, width:].astype(packed_ref.dtype)
    for k in range(copies):
        packed_ref[k, :value_rows, :] = value
        packed_ref[k, value_rows : value_rows + output_rows, :] = left
        packed_ref[k, value_rows + output_rows :, :] = right


def packed_copies(value_master, output_master, copies):
    value_rows, width = value_master.shape
    rows = value_rows + 2 * output_master.shape[0]
    return pl.pallas_call(
        pack_kernel,
        out_shape=jax.ShapeDtypeStruct((copies, rows, width), jnp.bfloat16),
        name="pack",
    )(value_master, output_master)


def project_kernel(index_ref, input_ref, mixer_ref, features_ref, heads_ref, partial_ref):
    blocks, tokens, width = partial_ref.shape
    partial = jnp.dot(input_ref[...], features_ref[...], preferred_element_type=jnp.float32)
    partial_ref[:, :, :R] = partial.astype(jnp.bfloat16).reshape(blocks, tokens, R)
    partial = jnp.dot(mixer_ref[...], heads_ref[...], preferred_element_type=jnp.float32)
    partial_ref[:, :, R:] = partial.astype(jnp.bfloat16).reshape(blocks, tokens, R)


def projected_tokens(index, normed_input, mixer_output, value_factor, output_factor, blocks):
    tokens, features = normed_input.shape
    heads = mixer_output.shape[1]
    return pl.pallas_call(
        project_kernel,
        grid_spec=pltpu.PrefetchScalarGridSpec(
            num_scalar_prefetch=1,
            grid=(1,),
            in_specs=[
                pl.BlockSpec((tokens, features), lambda i, index: (0, 0)),
                pl.BlockSpec((tokens, heads), lambda i, index: (0, 0)),
                pl.BlockSpec((features, R), lambda i, index: (index[0], 0)),
                pl.BlockSpec((heads, R), lambda i, index: (index[0], 0)),
            ],
            out_specs=pl.BlockSpec((blocks, tokens // blocks, 2 * R), lambda i, index: (0, 0, 0)),
        ),
        out_shape=jax.ShapeDtypeStruct((blocks, tokens // blocks, 2 * R), jnp.bfloat16),
        cost_estimate=pl.CostEstimate(
            flops=2 * tokens * (features + heads) * R,
            bytes_accessed=2 * tokens * (features + heads + 2 * R),
            transcendentals=0,
        ),
        name="project",
    )(index, normed_input, mixer_output, value_factor, output_factor)


def norms_kernel(
    gradient_ref,
    value_moment_ref,
    value_second_ref,
    output_moment_ref,
    output_second_ref,
    norm_ref,
    totals_ref,
):
    value_cols = value_moment_ref.shape[1]
    gradient = gradient_ref[...].astype(jnp.float32).reshape(R, gradient_ref.shape[2])
    value_norm = moments(value_moment_ref[...], value_second_ref[...], gradient[:, :value_cols])[2]
    output_norm = moments(
        output_moment_ref[...], output_second_ref[...], gradient[:, value_cols:]
    )[2]
    norm_ref[:, :value_cols] = value_norm
    norm_ref[:, value_cols:] = output_norm
    copies, _, lanes = totals_ref.shape
    total = []
    for norm in (value_norm, output_norm):
        squares = jnp.sum(norm * norm, axis=0, keepdims=True)
        total.append(sum(squares[:, k : k + lanes] for k in range(0, norm.shape[1], lanes)))
    for k in range(copies):
        totals_ref[k] = jnp.zeros(totals_ref.shape[1:], jnp.float32)
        totals_ref[k, 0:1, :] = total[0]
        totals_ref[k, 1:2, :] = total[1]


def normed(gradient, value_moment, value_second, output_moment, output_second, copies):
    return pl.pallas_call(
        norms_kernel,
        out_shape=[
            jax.ShapeDtypeStruct((R, gradient.shape[2]), jnp.float32),
            jax.ShapeDtypeStruct((copies, 8, 128), jnp.float32),
        ],
        compiler_params=pltpu.CompilerParams(vmem_limit_bytes=8 << 20),
        name="norms",
    )(gradient, value_moment, value_second, output_moment, output_second)


def inverse_root(totals, row, count):
    total = jnp.sum(totals[row : row + 1, :], axis=1, keepdims=True)
    return lax.rsqrt(total / count + FLOOR)


def product(rows, pair_ref):
    return jnp.dot(
        jnp.concatenate([rows, rows], axis=1), pair_ref[...], preferred_element_type=jnp.float32
    )


def update_kernel(
    row_ref,
    totals_ref,
    norm_ref,
    output_factor_ref,
    value_master_ref,
    output_master_ref,
    value_factor_hbm,
    masters_hbm,
    value_step_hbm,
    value_new_hbm,
    value_copy_hbm,
    output_step_hbm,
    output_new_hbm,
    output_copy_hbm,
    masters,
    value_factor,
    value_here,
    value_copy,
    output_copy,
    value_step,
    value_new,
    output_step,
    output_new,
    value_pair,
    output_pair,
    in_sems,
    factor_sems,
    here_sem,
    value_sems,
    output_sems,
    own_sems,
):
    chunks = in_sems.shape[0]
    n_fs, _, width = masters.shape
    group = n_fs // chunks
    value_rows, value_cols = value_master_ref.shape
    output_rows = output_master_ref.shape[0]

    def block(k):
        return pl.ds(k * group, group)

    def arriving(k):
        return pltpu.make_async_copy(
            masters_hbm.at[block(k)], masters.at[block(k)], in_sems.at[k]
        )

    def leaving_value(k):
        rows = pl.ds(k * group * value_rows, group * value_rows)
        return pltpu.make_async_copy(value_copy.at[rows], value_copy_hbm.at[rows], value_sems.at[k])

    def leaving_output(k):
        rows = pl.ds(k * group * output_rows, group * output_rows)
        return pltpu.make_async_copy(
            output_copy.at[rows], output_copy_hbm.at[rows], output_sems.at[k]
        )

    def arriving_factor(k):
        rows = pl.ds(k * group * value_rows, group * value_rows)
        return pltpu.make_async_copy(value_factor_hbm.at[rows], value_factor.at[rows], factor_sems.at[k])

    row = row_ref[0]
    rows_here = pl.ds(pl.multiple_of(row * value_rows, value_rows), value_rows)
    here = pltpu.make_async_copy(value_factor_hbm.at[rows_here], value_here, here_sem)
    here.start()
    for k in range(chunks):
        arriving_factor(k).start()
        arriving(k).start()

    totals = jnp.sum(totals_ref[...], axis=0)
    value_scale = inverse_root(totals, 0, R * WIDTH)
    output_scale = inverse_root(totals, 1, R * D)
    for pair, norm, scale in (
        (value_pair, norm_ref[:, :value_cols], value_scale),
        (output_pair, norm_ref[:, value_cols:], output_scale),
    ):
        scaled = (-STEP_RATE * scale) * norm
        high = scaled.astype(jnp.bfloat16)
        pair[:R, :] = high
        pair[R:, :] = (scaled - high.astype(jnp.float32)).astype(jnp.bfloat16)

    here.wait()
    change = product(value_here[...], value_pair)
    value_step[...] = change * (-1.0 / STEP_RATE)
    value_new[...] = value_master_ref[...] + change
    output_here = output_factor_ref[
        pl.ds(pl.multiple_of(row * output_rows, output_rows), output_rows), :
    ]
    change = product(output_here, output_pair)
    output_step[...] = change * (-1.0 / STEP_RATE)
    output_new[...] = output_master_ref[...] + change
    own = [
        pltpu.make_async_copy(value_step, value_step_hbm, own_sems.at[0]),
        pltpu.make_async_copy(value_new, value_new_hbm, own_sems.at[1]),
        pltpu.make_async_copy(output_step, output_step_hbm, own_sems.at[2]),
        pltpu.make_async_copy(output_new, output_new_hbm, own_sems.at[3]),
    ]
    for copy in own:
        copy.start()

    for k in range(chunks):
        arriving_factor(k).wait()
        arriving(k).wait()
        count = group * value_rows
        rows = slice(k * count, (k + 1) * count)
        mine = slice(k * group, (k + 1) * group)
        change = product(value_factor[rows, :], value_pair)
        old = masters[mine, :value_rows, :].reshape(count, width)
        value_copy[rows, :] = (old.astype(jnp.float32) + change).astype(jnp.bfloat16)
        leaving_value(k).start()
        count = group * output_rows
        rows = slice(k * count, (k + 1) * count)
        change = product(output_factor_ref[rows, :], output_pair)
        for side in range(2):
            first = value_rows + side * output_rows
            old = masters[mine, first : first + output_rows, :].reshape(count, width)
            columns = slice(side * width, (side + 1) * width)
            output_copy[rows, columns] = (old.astype(jnp.float32) + change[:, columns]).astype(
                jnp.bfloat16
            )
        leaving_output(k).start()

    for copy in own:
        copy.wait()
    for k in range(chunks):
        leaving_value(k).wait()
        leaving_output(k).wait()


def updated(
    row_index, totals, masters, value_factor, output_factor, norm, value_master, output_master
):
    n_fs, packed_rows, width = masters.shape
    chunks = 4
    value_rows, value_cols = value_master.shape
    output_rows, output_cols = output_master.shape
    in_vmem = pl.BlockSpec(memory_space=pltpu.VMEM)
    anywhere = pl.BlockSpec(memory_space=pl.ANY)
    outs = [
        jax.ShapeDtypeStruct(value_master.shape, jnp.float32),
        jax.ShapeDtypeStruct(value_master.shape, jnp.float32),
        jax.ShapeDtypeStruct((n_fs * value_rows, value_cols), jnp.bfloat16),
        jax.ShapeDtypeStruct(output_master.shape, jnp.float32),
        jax.ShapeDtypeStruct(output_master.shape, jnp.float32),
        jax.ShapeDtypeStruct((n_fs * output_rows, output_cols), jnp.bfloat16),
    ]
    return pl.pallas_call(
        update_kernel,
        in_specs=[pl.BlockSpec(memory_space=pltpu.SMEM)] + [in_vmem] * 5 + [anywhere] * 2,
        out_specs=[anywhere] * 6,
        out_shape=outs,
        scratch_shapes=[
            pltpu.VMEM(masters.shape, jnp.bfloat16),
            pltpu.VMEM(value_factor.shape, jnp.bfloat16),
            pltpu.VMEM((value_rows, R), jnp.bfloat16),
            pltpu.VMEM(outs[2].shape, jnp.bfloat16),
            pltpu.VMEM(outs[5].shape, jnp.bfloat16),
            pltpu.VMEM(value_master.shape, jnp.float32),
            pltpu.VMEM(value_master.shape, jnp.float32),
            pltpu.VMEM(output_master.shape, jnp.float32),
            pltpu.VMEM(output_master.shape, jnp.float32),
            pltpu.VMEM((2 * R, value_cols), jnp.bfloat16),
            pltpu.VMEM((2 * R, output_cols), jnp.bfloat16),
            pltpu.SemaphoreType.DMA((chunks,)),
            pltpu.SemaphoreType.DMA((chunks,)),
            pltpu.SemaphoreType.DMA,
            pltpu.SemaphoreType.DMA((chunks,)),
            pltpu.SemaphoreType.DMA((chunks,)),
            pltpu.SemaphoreType.DMA((4,)),
        ],
        cost_estimate=pl.CostEstimate(
            flops=4 * R * n_fs * (value_rows * value_cols + output_rows * output_cols),
            bytes_accessed=4 * n_fs * packed_rows * width,
            transcendentals=0,
        ),
        compiler_params=pltpu.CompilerParams(vmem_limit_bytes=52 << 20),
        name="update",
    )(
        row_index,
        totals,
        norm,
        output_factor,
        value_master,
        output_master,
        value_factor,
        masters,
    )


def per_device(
    normed_input,
    value_cotangent,
    mixer_output,
    output_cotangent,
    value_factor,
    output_factor,
    value_master,
    value_moment,
    value_second,
    output_master,
    output_moment,
    output_second,
):
    row_index = lax.axis_index(FS).reshape(1)
    column_index = lax.axis_index("tp").reshape(1)
    n_fs = lax.axis_size(FS)
    n_tp = lax.axis_size("tp")
    tokens = normed_input.shape[0]

    packed = packed_copies(value_master, output_master, lax.axis_size("y"))
    plane = lax.all_to_all(packed, "y", split_axis=0, concat_axis=0, tiled=True)

    partial = projected_tokens(
        column_index, normed_input, mixer_output, value_factor, output_factor, n_tp
    )
    partial, plane, row_index = lax.optimization_barrier((partial, plane, row_index))
    masters = lax.all_gather(plane, Z).reshape(n_fs, *packed.shape[1:])
    blocks = lax.all_to_all(partial, "tp", split_axis=0, concat_axis=0, tiled=True)
    own = jnp.sum(blocks.astype(jnp.float32), axis=0).astype(jnp.bfloat16)
    reduced = sent_to_all(own, "tp").reshape(tokens, 2 * R)

    value_partial = contract_rows(reduced[:, :R], value_cotangent)
    output_partial = contract_rows(reduced[:, R:], output_cotangent)
    n_y, n_zl = lax.axis_size("y"), lax.axis_size("zl")
    gradient = jnp.concatenate([value_partial, output_partial], axis=1)
    gradient = gradient.reshape(n_y, R // n_y, -1)
    gradient = lax.all_to_all(gradient, "y", split_axis=0, concat_axis=0, tiled=True)
    gradient = jnp.sum(gradient, axis=0).reshape(n_zl, R // n_y // n_zl, -1)
    gradient = lax.all_to_all(gradient, "zl", split_axis=0, concat_axis=0, tiled=True)
    gradient = jnp.sum(gradient, axis=0)
    gradient = summed_far(gradient, FAR)
    gradient = sent_to_all(gradient.astype(jnp.bfloat16), ("y", "zl"))

    norm, totals = normed(
        gradient, value_moment, value_second, output_moment, output_second, n_tp
    )
    flat = gradient.astype(jnp.float32).reshape(R, -1)
    value_cols = value_master.shape[1]
    value_moment_new, value_second_new, _ = moments(
        value_moment, value_second, flat[:, :value_cols]
    )
    output_moment_new, output_second_new, _ = moments(
        output_moment, output_second, flat[:, value_cols:]
    )
    totals = lax.all_to_all(totals, "tp", split_axis=0, concat_axis=0, tiled=True)
    value_step, value_new, value_copy, output_step, output_new, output_copy = updated(
        row_index, totals, masters, value_factor, output_factor, norm, value_master, output_master
    )
    return (
        value_step,
        value_new,
        value_copy,
        value_moment_new,
        value_second_new,
        output_step,
        output_new,
        output_copy,
        output_moment_new,
        output_second_new,
    )


def solution(mesh):
    finer = Mesh(mesh.devices.reshape(4, 4, 4, mesh.shape["tp"]), ("zh", "zl", "y", "tp"))
    placed = (
        P(FS, "tp"),
        P(FS, "tp"),
        P(FS, "tp"),
        P(FS, "tp"),
        P(),
        P(),
        P(FS, "tp"),
        P(None, "tp"),
        P(None, "tp"),
        P(FS, "tp"),
        P(None, "tp"),
        P(None, "tp"),
    )
    return jax.shard_map(
        per_device,
        mesh=finer,
        in_specs=placed,
        out_specs=(
            P(FS, "tp"),
            P(FS, "tp"),
            P(None, "tp"),
            P(None, "tp"),
            P(None, "tp"),
            P(FS, "tp"),
            P(FS, "tp"),
            P(None, "tp"),
            P(None, "tp"),
            P(None, "tp"),
        ),
        check_vma=False,
    )
```

```python
import jax
import jax.numpy as jnp
from jax import lax
from jax.experimental import pallas as pl
from jax.experimental.pallas import tpu as pltpu
from jax.sharding import Mesh
from jax.sharding import PartitionSpec as P

D = 4096
WIDTH = 2048
R = 128
FS = ("zh", "zl", "y")
Z = ("zh", "zl")
NEAR = ("zl", "y")
FAR = "zh"

BETA_ONE = 0.8
BETA_TWO = 0.9
EPSILON = 1e-08
STEP_RATE = 0.005
FLOOR = 0.25


def sent_to_all(shard, axis):
    copies = jnp.broadcast_to(shard, (lax.axis_size(axis), *shard.shape))
    return lax.all_to_all(copies, axis, split_axis=0, concat_axis=0, tiled=True)


def summed_far(part, axis):
    size = lax.axis_size(axis)
    for by in (size // 2, 1):
        part = part + lax.ppermute(part, axis, [(i, i ^ by) for i in range(size)])
    return part


def contract_rows(left, right):
    return lax.dot_general(
        left, right, (((0,), (0,)), ((), ())), preferred_element_type=jnp.float32
    )


def moments(first, second, projected):
    first_new = BETA_ONE * first + (1.0 - BETA_ONE) * projected
    second_new = BETA_TWO * second + (1.0 - BETA_TWO) * projected * projected
    normalized = first_new / (jnp.sqrt(second_new) + EPSILON)
    return (first_new, second_new, normalized)


def pack_kernel(value_ref, output_ref, packed_ref):
    copies, packed_rows, width = packed_ref.shape
    value_rows = value_ref.shape[0]
    output_rows = output_ref.shape[0]
    value = value_ref[...].astype(packed_ref.dtype)
    left = output_ref[:, :width].astype(packed_ref.dtype)
    right = output_ref[:, width:].astype(packed_ref.dtype)
    for k in range(copies):
        packed_ref[k, :value_rows, :] = value
        packed_ref[k, value_rows : value_rows + output_rows, :] = left
        packed_ref[k, value_rows + output_rows :, :] = right


def packed_copies(value_master, output_master, copies):
    value_rows, width = value_master.shape
    rows = value_rows + 2 * output_master.shape[0]
    return pl.pallas_call(
        pack_kernel,
        out_shape=jax.ShapeDtypeStruct((copies, rows, width), jnp.bfloat16),
        name="pack",
    )(value_master, output_master)


def project_kernel(index_ref, input_ref, mixer_ref, features_ref, heads_ref, partial_ref):
    blocks, tokens, width = partial_ref.shape
    partial = jnp.dot(input_ref[...], features_ref[...], preferred_element_type=jnp.float32)
    partial_ref[:, :, :R] = partial.astype(jnp.bfloat16).reshape(blocks, tokens, R)
    partial = jnp.dot(mixer_ref[...], heads_ref[...], preferred_element_type=jnp.float32)
    partial_ref[:, :, R:] = partial.astype(jnp.bfloat16).reshape(blocks, tokens, R)


def projected_tokens(index, normed_input, mixer_output, value_factor, output_factor, blocks):
    tokens, features = normed_input.shape
    heads = mixer_output.shape[1]
    return pl.pallas_call(
        project_kernel,
        grid_spec=pltpu.PrefetchScalarGridSpec(
            num_scalar_prefetch=1,
            grid=(1,),
            in_specs=[
                pl.BlockSpec((tokens, features), lambda i, index: (0, 0)),
                pl.BlockSpec((tokens, heads), lambda i, index: (0, 0)),
                pl.BlockSpec((features, R), lambda i, index: (index[0], 0)),
                pl.BlockSpec((heads, R), lambda i, index: (index[0], 0)),
            ],
            out_specs=pl.BlockSpec((blocks, tokens // blocks, 2 * R), lambda i, index: (0, 0, 0)),
        ),
        out_shape=jax.ShapeDtypeStruct((blocks, tokens // blocks, 2 * R), jnp.bfloat16),
        cost_estimate=pl.CostEstimate(
            flops=2 * tokens * (features + heads) * R,
            bytes_accessed=2 * tokens * (features + heads + 2 * R),
            transcendentals=0,
        ),
        name="project",
    )(index, normed_input, mixer_output, value_factor, output_factor)


def norms_kernel(
    gradient_ref,
    value_moment_ref,
    value_second_ref,
    output_moment_ref,
    output_second_ref,
    norm_ref,
    totals_ref,
):
    value_cols = value_moment_ref.shape[1]
    gradient = gradient_ref[...].astype(jnp.float32).reshape(R, gradient_ref.shape[2])
    value_norm = moments(value_moment_ref[...], value_second_ref[...], gradient[:, :value_cols])[2]
    output_norm = moments(
        output_moment_ref[...], output_second_ref[...], gradient[:, value_cols:]
    )[2]
    norm_ref[:, :value_cols] = value_norm
    norm_ref[:, value_cols:] = output_norm
    copies, _, lanes = totals_ref.shape
    total = []
    for norm in (value_norm, output_norm):
        squares = jnp.sum(norm * norm, axis=0, keepdims=True)
        total.append(sum(squares[:, k : k + lanes] for k in range(0, norm.shape[1], lanes)))
    for k in range(copies):
        totals_ref[k] = jnp.zeros(totals_ref.shape[1:], jnp.float32)
        totals_ref[k, 0:1, :] = total[0]
        totals_ref[k, 1:2, :] = total[1]


def normed(gradient, value_moment, value_second, output_moment, output_second, copies):
    return pl.pallas_call(
        norms_kernel,
        out_shape=[
            jax.ShapeDtypeStruct((R, gradient.shape[2]), jnp.float32),
            jax.ShapeDtypeStruct((copies, 8, 128), jnp.float32),
        ],
        compiler_params=pltpu.CompilerParams(vmem_limit_bytes=8 << 20),
        name="norms",
    )(gradient, value_moment, value_second, output_moment, output_second)


def inverse_root(totals, row, count):
    total = jnp.sum(totals[row : row + 1, :], axis=1, keepdims=True)
    return lax.rsqrt(total / count + FLOOR)


def product(rows, pair_ref):
    return jnp.dot(
        jnp.concatenate([rows, rows], axis=1), pair_ref[...], preferred_element_type=jnp.float32
    )


def chunked(count):
    part = count // 8
    sizes = [part, 2 * part, 2 * part, 2 * part, count - 7 * part]
    return [sum(sizes[:k]) for k in range(len(sizes))], sizes


def update_kernel(
    row_ref,
    totals_ref,
    norm_ref,
    output_factor_ref,
    value_master_ref,
    output_master_ref,
    value_factor_hbm,
    masters_hbm,
    value_step_hbm,
    value_new_hbm,
    value_copy_hbm,
    output_step_hbm,
    output_new_hbm,
    output_copy_hbm,
    masters,
    value_factor,
    value_here,
    value_copy,
    output_copy,
    value_step,
    value_new,
    output_step,
    output_new,
    value_pair,
    output_pair,
    in_sems,
    factor_sems,
    here_sem,
    value_sems,
    output_sems,
    own_sems,
):
    n_fs, _, width = masters.shape
    starts, sizes = chunked(n_fs)
    chunks = len(sizes)
    value_rows, value_cols = value_master_ref.shape
    output_rows = output_master_ref.shape[0]

    def block(k):
        return pl.ds(starts[k], sizes[k])

    def arriving(k):
        return pltpu.make_async_copy(
            masters_hbm.at[block(k)], masters.at[block(k)], in_sems.at[k]
        )

    def leaving_value(k):
        rows = pl.ds(starts[k] * value_rows, sizes[k] * value_rows)
        return pltpu.make_async_copy(value_copy.at[rows], value_copy_hbm.at[rows], value_sems.at[k])

    def leaving_output(k):
        rows = pl.ds(starts[k] * output_rows, sizes[k] * output_rows)
        return pltpu.make_async_copy(
            output_copy.at[rows], output_copy_hbm.at[rows], output_sems.at[k]
        )

    def arriving_factor(k):
        rows = pl.ds(starts[k] * value_rows, sizes[k] * value_rows)
        return pltpu.make_async_copy(value_factor_hbm.at[rows], value_factor.at[rows], factor_sems.at[k])

    row = row_ref[0]
    rows_here = pl.ds(pl.multiple_of(row * value_rows, value_rows), value_rows)
    here = pltpu.make_async_copy(value_factor_hbm.at[rows_here], value_here, here_sem)
    here.start()
    for k in range(chunks):
        arriving_factor(k).start()
        arriving(k).start()

    totals = jnp.sum(totals_ref[...], axis=0)
    value_scale = inverse_root(totals, 0, R * WIDTH)
    output_scale = inverse_root(totals, 1, R * D)
    for pair, norm, scale in (
        (value_pair, norm_ref[:, :value_cols], value_scale),
        (output_pair, norm_ref[:, value_cols:], output_scale),
    ):
        scaled = (-STEP_RATE * scale) * norm
        high = scaled.astype(jnp.bfloat16)
        pair[:R, :] = high
        pair[R:, :] = (scaled - high.astype(jnp.float32)).astype(jnp.bfloat16)

    here.wait()
    change = product(value_here[...], value_pair)
    value_step[...] = change * (-1.0 / STEP_RATE)
    value_new[...] = value_master_ref[...] + change
    output_here = output_factor_ref[
        pl.ds(pl.multiple_of(row * output_rows, output_rows), output_rows), :
    ]
    change = product(output_here, output_pair)
    output_step[...] = change * (-1.0 / STEP_RATE)
    output_new[...] = output_master_ref[...] + change
    own = [
        pltpu.make_async_copy(value_step, value_step_hbm, own_sems.at[0]),
        pltpu.make_async_copy(value_new, value_new_hbm, own_sems.at[1]),
        pltpu.make_async_copy(output_step, output_step_hbm, own_sems.at[2]),
        pltpu.make_async_copy(output_new, output_new_hbm, own_sems.at[3]),
    ]
    for copy in own:
        copy.start()

    for k in range(chunks):
        arriving_factor(k).wait()
        arriving(k).wait()
        count = sizes[k] * value_rows
        rows = slice(starts[k] * value_rows, starts[k] * value_rows + count)
        mine = slice(starts[k], starts[k] + sizes[k])
        change = product(value_factor[rows, :], value_pair)
        old = masters[mine, :value_rows, :].reshape(count, width)
        value_copy[rows, :] = (old.astype(jnp.float32) + change).astype(jnp.bfloat16)
        leaving_value(k).start()
        count = sizes[k] * output_rows
        rows = slice(starts[k] * output_rows, starts[k] * output_rows + count)
        change = product(output_factor_ref[rows, :], output_pair)
        for side in range(2):
            first = value_rows + side * output_rows
            old = masters[mine, first : first + output_rows, :].reshape(count, width)
            columns = slice(side * width, (side + 1) * width)
            output_copy[rows, columns] = (old.astype(jnp.float32) + change[:, columns]).astype(
                jnp.bfloat16
            )
        leaving_output(k).start()

    for copy in own:
        copy.wait()
    for k in range(chunks):
        leaving_value(k).wait()
        leaving_output(k).wait()


def updated(
    row_index, totals, masters, value_factor, output_factor, norm, value_master, output_master
):
    n_fs, packed_rows, width = masters.shape
    chunks = len(chunked(n_fs)[1])
    value_rows, value_cols = value_master.shape
    output_rows, output_cols = output_master.shape
    in_vmem = pl.BlockSpec(memory_space=pltpu.VMEM)
    anywhere = pl.BlockSpec(memory_space=pl.ANY)
    outs = [
        jax.ShapeDtypeStruct(value_master.shape, jnp.float32),
        jax.ShapeDtypeStruct(value_master.shape, jnp.float32),
        jax.ShapeDtypeStruct((n_fs * value_rows, value_cols), jnp.bfloat16),
        jax.ShapeDtypeStruct(output_master.shape, jnp.float32),
        jax.ShapeDtypeStruct(output_master.shape, jnp.float32),
        jax.ShapeDtypeStruct((n_fs * output_rows, output_cols), jnp.bfloat16),
    ]
    return pl.pallas_call(
        update_kernel,
        in_specs=[pl.BlockSpec(memory_space=pltpu.SMEM)] + [in_vmem] * 5 + [anywhere] * 2,
        out_specs=[anywhere] * 6,
        out_shape=outs,
        scratch_shapes=[
            pltpu.VMEM(masters.shape, jnp.bfloat16),
            pltpu.VMEM(value_factor.shape, jnp.bfloat16),
            pltpu.VMEM((value_rows, R), jnp.bfloat16),
            pltpu.VMEM(outs[2].shape, jnp.bfloat16),
            pltpu.VMEM(outs[5].shape, jnp.bfloat16),
            pltpu.VMEM(value_master.shape, jnp.float32),
            pltpu.VMEM(value_master.shape, jnp.float32),
            pltpu.VMEM(output_master.shape, jnp.float32),
            pltpu.VMEM(output_master.shape, jnp.float32),
            pltpu.VMEM((2 * R, value_cols), jnp.bfloat16),
            pltpu.VMEM((2 * R, output_cols), jnp.bfloat16),
            pltpu.SemaphoreType.DMA((chunks,)),
            pltpu.SemaphoreType.DMA((chunks,)),
            pltpu.SemaphoreType.DMA,
            pltpu.SemaphoreType.DMA((chunks,)),
            pltpu.SemaphoreType.DMA((chunks,)),
            pltpu.SemaphoreType.DMA((4,)),
        ],
        cost_estimate=pl.CostEstimate(
            flops=4 * R * n_fs * (value_rows * value_cols + output_rows * output_cols),
            bytes_accessed=4 * n_fs * packed_rows * width,
            transcendentals=0,
        ),
        compiler_params=pltpu.CompilerParams(vmem_limit_bytes=52 << 20),
        name="update",
    )(
        row_index,
        totals,
        norm,
        output_factor,
        value_master,
        output_master,
        value_factor,
        masters,
    )


def per_device(
    normed_input,
    value_cotangent,
    mixer_output,
    output_cotangent,
    value_factor,
    output_factor,
    value_master,
    value_moment,
    value_second,
    output_master,
    output_moment,
    output_second,
):
    row_index = lax.axis_index(FS).reshape(1)
    column_index = lax.axis_index("tp").reshape(1)
    n_fs = lax.axis_size(FS)
    n_tp = lax.axis_size("tp")
    tokens = normed_input.shape[0]

    packed = packed_copies(value_master, output_master, lax.axis_size("y"))
    plane = lax.all_to_all(packed, "y", split_axis=0, concat_axis=0, tiled=True)

    partial = projected_tokens(
        column_index, normed_input, mixer_output, value_factor, output_factor, n_tp
    )
    partial, plane, row_index = lax.optimization_barrier((partial, plane, row_index))
    masters = lax.all_gather(plane, Z).reshape(n_fs, *packed.shape[1:])
    blocks = lax.all_to_all(partial, "tp", split_axis=0, concat_axis=0, tiled=True)
    own = jnp.sum(blocks.astype(jnp.float32), axis=0).astype(jnp.bfloat16)
    reduced = sent_to_all(own, "tp").reshape(tokens, 2 * R)

    value_partial = contract_rows(reduced[:, :R], value_cotangent)
    output_partial = contract_rows(reduced[:, R:], output_cotangent)
    n_y, n_zl = lax.axis_size("y"), lax.axis_size("zl")
    gradient = jnp.concatenate([value_partial, output_partial], axis=1)
    gradient = gradient.reshape(n_y, R // n_y, -1)
    gradient = lax.all_to_all(gradient, "y", split_axis=0, concat_axis=0, tiled=True)
    gradient = jnp.sum(gradient, axis=0).reshape(n_zl, R // n_y // n_zl, -1)
    gradient = lax.all_to_all(gradient, "zl", split_axis=0, concat_axis=0, tiled=True)
    gradient = jnp.sum(gradient, axis=0)
    gradient = summed_far(gradient, FAR)
    gradient = sent_to_all(gradient.astype(jnp.bfloat16), ("y", "zl"))

    norm, totals = normed(
        gradient, value_moment, value_second, output_moment, output_second, n_tp
    )
    flat = gradient.astype(jnp.float32).reshape(R, -1)
    value_cols = value_master.shape[1]
    value_moment_new, value_second_new, _ = moments(
        value_moment, value_second, flat[:, :value_cols]
    )
    output_moment_new, output_second_new, _ = moments(
        output_moment, output_second, flat[:, value_cols:]
    )
    totals = lax.all_to_all(totals, "tp", split_axis=0, concat_axis=0, tiled=True)
    value_step, value_new, value_copy, output_step, output_new, output_copy = updated(
        row_index, totals, masters, value_factor, output_factor, norm, value_master, output_master
    )
    return (
        value_step,
        value_new,
        value_copy,
        value_moment_new,
        value_second_new,
        output_step,
        output_new,
        output_copy,
        output_moment_new,
        output_second_new,
    )


def solution(mesh):
    finer = Mesh(mesh.devices.reshape(4, 4, 4, mesh.shape["tp"]), ("zh", "zl", "y", "tp"))
    placed = (
        P(FS, "tp"),
        P(FS, "tp"),
        P(FS, "tp"),
        P(FS, "tp"),
        P(),
        P(),
        P(FS, "tp"),
        P(None, "tp"),
        P(None, "tp"),
        P(FS, "tp"),
        P(None, "tp"),
        P(None, "tp"),
    )
    return jax.shard_map(
        per_device,
        mesh=finer,
        in_specs=placed,
        out_specs=(
            P(FS, "tp"),
            P(FS, "tp"),
            P(None, "tp"),
            P(None, "tp"),
            P(None, "tp"),
            P(FS, "tp"),
            P(FS, "tp"),
            P(None, "tp"),
            P(None, "tp"),
            P(None, "tp"),
        ),
        check_vma=False,
    )
```
